32 devices in a mesh: sp: 8 (over z, x), tp: 4 (over y, core).
Axes of the slice: x: 2, y: 2, z: 4, core: 2. Of those that a mesh axis runs over, the one named last changes fastest.
Arguments:
- queries: bfloat16 [4096, 2048], P('sp', 'tp'), may hold values from -90 to 90, as said below
- key_rows: bfloat16 [4096, 512], P('sp', 'tp'), may hold values from -6 to 6
- value_rows: bfloat16 [4096, 512], P('sp', 'tp'), may hold values from -6 to 6
- sink_logits: float32 [16], P('tp'), may hold values from 2 to 7
- residual: bfloat16 [4096, 2048], P('sp'), may hold values from -6 to 6
- norm_gain: float32 [2048], replicated, may hold values from 0.1 to 1.9
- out_weight: bfloat16 [2048, 2048], P('tp'), may hold values from -1.5 to 1.5
- gate_weight: bfloat16 [2048, 5632], P('sp', 'tp'), may hold values from -0.125 to 0.125
- up_weight: bfloat16 [2048, 5632], P('sp', 'tp'), may hold values from -0.125 to 0.125
- down_weight: bfloat16 [5632, 2048], P('tp', 'sp'), may hold values from -0.078125 to 0.078125
Outputs:
- mixed: bfloat16 [4096, 2048], P(('sp', 'tp'))
The draws below stay inside these ranges and needn't reach their ends.
Inputs may be any that keep to these rules, and one draw needn't show every extreme that they name: queries are mostly of order one; some rows may be much larger.
All inputs are finite; a program needn't handle non-finite values.
Results may differ from the reference program's by a relative error of at most 0.012.
Values may be sent and summed in bfloat16 or wider, within the bound.
No kernel may reach another device: no remote copies, remote signals or barrier semaphores. Data moves between devices by JAX's collectives and lax.ppermute only.
A program may use at most 128 MiB of HBM per device.

```python
import jax
import jax.numpy as jnp
from jax import lax

D = 2048
HQ = 16
HK = 4
DH = 128
FF = 5632
WIN = 128
TOKENS = 4096
N_TP = 4


def shared_draws(key):
    base = jax.random.fold_in(key, 11)
    key_query, key_keys = jax.random.split(base, 2)
    keys_wide = jnp.clip(jax.random.normal(key_keys, (TOKENS, HK * DH), jnp.float32), -5.0, 5.0)
    query_wide = jnp.clip(jax.random.normal(key_query, (TOKENS, HQ * DH), jnp.float32), -5.0, 5.0)
    return (query_wide, keys_wide)


def draw_queries(key, part):
    return shared_draws(key)[0].astype(jnp.bfloat16)


def draw_key_rows(key, part):
    return shared_draws(key)[1].astype(jnp.bfloat16)


def steps_of(stream_key, shape, cuts, smallest, largest):
    def one(position, shards_of):
        steps = jax.random.uniform(jax.random.fold_in(jax.random.fold_in(stream_key, 6), position), (shards_of,), jnp.float32, smallest / len(cuts), largest / len(cuts))
        return jnp.repeat(jnp.exp(steps), shape[position] // shards_of).reshape((-1,) + (1,) * (len(shape) - position - 1))

    factor_of = one(*cuts[0])
    for cut in cuts[1:]:
        factor_of = factor_of * one(*cut)
    return factor_of


def gaussian(stream_key, dims, spread, most, pieces=(), kind=jnp.bfloat16):
    level = steps_of(stream_key, dims, pieces, -0.22, 0.18) if pieces else 1.0
    values = jax.random.normal(stream_key, dims, jnp.float32) * spread * level
    return jnp.minimum(jnp.maximum(values, -most), most).astype(kind)


def setup_inputs(seed: int = 0) -> dict:
    key_of = jax.random.split(jax.random.key(seed), 11)
    return {
        "queries": draw_queries(jax.random.fold_in(key_of[10], 71), 0),
        "key_rows": draw_key_rows(jax.random.fold_in(key_of[10], 71), 0),
        "value_rows": gaussian(key_of[2], (TOKENS, HK * DH), 1.0, 6.0, ((0, 8), (1, 4))),
        "sink_logits": jnp.clip(2.0 + 5.0 * jax.random.uniform(key_of[3], (HQ,), jnp.float32) ** steps_of(key_of[3], (HQ,), ((0, 4),), -0.2, 0.2), 2.0, 7.0),
        "residual": gaussian(key_of[4], (TOKENS, D), 1.0, 6.0, ((0, 8),)),
        "norm_gain": jnp.clip(1.0 + 0.18 * jax.random.normal(key_of[5], (D,), jnp.float32), 0.1, 1.9),
        "out_weight": gaussian(key_of[6], (HQ * DH, D), 0.25, 1.5, ((0, 4),)),
        "gate_weight": gaussian(key_of[7], (D, FF), D ** -0.5, 0.125, ((0, 8), (1, 4))),
        "up_weight": gaussian(key_of[8], (D, FF), D ** -0.5, 0.125, ((0, 8), (1, 4))),
        "down_weight": gaussian(key_of[9], (FF, D), FF ** -0.5, 0.078125, ((0, 4), (1, 8))),
    }


EPSILON = 1e-06
MASKED = -1e+30

def attend_block(query_blk, key_blk, value_blk, sink_logits, query_pos, key_pos, seq_len):
    kv_heads = key_blk.shape[1] // DH
    group_size = query_blk.shape[1] // key_blk.shape[1]
    query_four = query_blk.reshape(query_blk.shape[0], kv_heads, group_size, DH).astype(jnp.float32)
    key_three = key_blk.reshape(key_blk.shape[0], kv_heads, DH).astype(jnp.float32)
    value_three = value_blk.reshape(value_blk.shape[0], kv_heads, DH).astype(jnp.float32)
    scores = jnp.einsum('qhgd,khd->hgqk', query_four, key_three) * DH ** (-0.5)
    allowed = (jnp.abs(key_pos[None, :] - query_pos[:, None]) <= WIN) & (key_pos[None, :] >= 0) & (key_pos[None, :] < seq_len)
    scores = jnp.where(allowed[None, None], scores, MASKED)
    sink_col = sink_logits.astype(jnp.float32).reshape(kv_heads, group_size)[:, :, None]
    highest = jnp.maximum(lax.optimization_barrier(jnp.max(scores, axis=-1)), sink_col)
    weights_exp = jnp.exp(scores - highest[..., None])
    denominator = lax.optimization_barrier(jnp.sum(weights_exp, axis=-1)) + jnp.exp(sink_col - highest)
    probabilities = (weights_exp / denominator[..., None]).astype(jnp.bfloat16)
    heads_out = jnp.einsum('hgqk,khd->qhgd', probabilities.astype(jnp.float32), value_three)
    return heads_out.astype(jnp.bfloat16).reshape(query_blk.shape[0], kv_heads * group_size * DH)

def rms_scale(rows_wide, norm_gain):
    mean_square = lax.optimization_barrier(jnp.mean(rows_wide * rows_wide, axis=-1, keepdims=True))
    return (rows_wide * lax.rsqrt(mean_square + EPSILON) * norm_gain).astype(jnp.bfloat16)

def grouped_sum(left, right, group_cols):
    result = jnp.zeros((left.shape[0], right.shape[1]), jnp.float32)
    for group_index in range(N_TP):
        lower = group_index * group_cols
        partial_term = jnp.dot(left[:, lower:lower + group_cols], right[lower:lower + group_cols], preferred_element_type=jnp.float32)
        rounded = lax.optimization_barrier(partial_term.astype(jnp.bfloat16))
        result = result + rounded.astype(jnp.float32)
    return result

def reference(queries, key_rows, value_rows, sink_logits, residual, norm_gain, out_weight, gate_weight, up_weight, down_weight):
    block_len = 2 * WIN
    key_pad = jnp.pad(key_rows, ((WIN, WIN), (0, 0)))
    value_pad = jnp.pad(value_rows, ((WIN, WIN), (0, 0)))

    def one_block(block_index):
        block_first = (block_index * block_len).astype(jnp.int32)
        query_blk = lax.dynamic_slice_in_dim(queries, block_first, block_len, 0)
        key_blk = lax.dynamic_slice_in_dim(key_pad, block_first, block_len + 2 * WIN, 0)
        value_blk = lax.dynamic_slice_in_dim(value_pad, block_first, block_len + 2 * WIN, 0)
        query_pos = block_first + jnp.arange(block_len, dtype=jnp.int32)
        key_pos = block_first - WIN + jnp.arange(block_len + 2 * WIN, dtype=jnp.int32)
        return attend_block(query_blk, key_blk, value_blk, sink_logits, query_pos, key_pos, TOKENS)
    blocks = lax.map(one_block, jnp.arange(TOKENS // block_len, dtype=jnp.int32))
    attended = blocks.reshape(TOKENS, HQ * DH)
    attn_total = grouped_sum(attended, out_weight, HQ * DH // N_TP)
    middle = residual.astype(jnp.float32) + attn_total
    normed = rms_scale(middle, norm_gain)
    gate_acc = jnp.dot(normed, gate_weight, preferred_element_type=jnp.float32)
    up_acc = jnp.dot(normed, up_weight, preferred_element_type=jnp.float32)
    hidden = (jax.nn.silu(gate_acc) * up_acc).astype(jnp.bfloat16)
    ffn_total = grouped_sum(hidden, down_weight, FF // N_TP)
    return (middle + ffn_total).astype(jnp.bfloat16)
```

```python
import jax
import jax.numpy as jnp
from jax import lax
from jax.sharding import PartitionSpec as P

DH = 128
WIN = 128
LANES = 128


EPSILON = 1e-06
MASKED = -1e30


class Layout:
    def __init__(self, n_sp, n_tp):
        self.n_sp = n_sp
        self.n_tp = n_tp
        self.far = n_sp // 4
        self.ranks = n_tp // 2

    def split(self, flat):
        s, t = flat // self.n_tp, flat % self.n_tp
        return s // 4, (s // 2) % 2, s % 2, t // 2, t % 2

    def join(self, far, near, side, rank, core):
        return ((far * 2 + near) * 2 + side) * self.n_tp + rank * 2 + core

    def pairs(self, move):
        out = []
        for flat in range(self.n_sp * self.n_tp):
            out.append((flat, self.join(*move(*self.split(flat)))))
        return out


def send(cells, pairs):
    return lax.ppermute(cells, ("sp", "tp"), pairs)


def halo(cells):
    count = lax.axis_size("sp")
    head, tail = cells[:, :WIN], cells[:, cells.shape[1] - WIN :]
    before = lax.ppermute(tail, "sp", [(i, i + 1) for i in range(count - 1)])
    after = lax.ppermute(head, "sp", [(i + 1, i) for i in range(count - 1)])
    return jnp.concatenate([before, cells, after], axis=1)


def attend_block(query_blk, key_blk, value_blk, sink_logits, query_pos, key_pos, seq_len):
    kv_heads = key_blk.shape[1] // DH
    group_size = query_blk.shape[1] // key_blk.shape[1]
    query_four = query_blk.reshape(query_blk.shape[0], kv_heads, group_size, DH)
    key_three = key_blk.reshape(key_blk.shape[0], kv_heads, DH)
    value_three = value_blk.reshape(value_blk.shape[0], kv_heads, DH)
    scores = jnp.einsum(
        "qhgd,khd->hgqk", query_four, key_three, preferred_element_type=jnp.float32
    ) * DH ** (-0.5)
    allowed = (
        (jnp.abs(key_pos[None, :] - query_pos[:, None]) <= WIN)
        & (key_pos[None, :] >= 0)
        & (key_pos[None, :] < seq_len)
    )
    scores = jnp.where(allowed[None, None], scores, MASKED)
    sink_col = sink_logits.reshape(kv_heads, group_size)[:, :, None]
    highest = jnp.maximum(jnp.max(scores, axis=-1), sink_col)
    weights_exp = jnp.exp(scores - highest[..., None])
    denominator = jnp.sum(weights_exp, axis=-1) + jnp.exp(sink_col - highest)
    probabilities = (weights_exp / denominator[..., None]).astype(jnp.bfloat16)
    heads_out = jnp.einsum(
        "hgqk,khd->qhgd", probabilities, value_three, preferred_element_type=jnp.float32
    )
    return heads_out.astype(jnp.bfloat16).reshape(query_blk.shape[0], kv_heads * group_size * DH)


def rms_scale(rows_wide, norm_gain):
    mean_square = jnp.mean(rows_wide * rows_wide, axis=-1, keepdims=True)
    return (rows_wide * lax.rsqrt(mean_square + EPSILON) * norm_gain).astype(jnp.bfloat16)


def gathered(
    queries,
    key_rows,
    value_rows,
    sink_logits,
    residual,
    norm_gain,
    out_weight,
    gate_weight,
    up_weight,
    down_weight,
):
    tok_local = queries.shape[0]
    block_len = 2 * WIN
    share_rows = tok_local // lax.axis_size("tp")
    seq_len = tok_local * lax.axis_size("sp")
    device_offset = lax.axis_index("sp") * tok_local
    kv_pair = jnp.stack([key_rows, value_rows])
    kv_ext = halo(kv_pair)

    def one_block(block_index):
        block_first = block_index * block_len
        query_blk = lax.dynamic_slice_in_dim(queries, block_first, block_len, 0)
        key_blk = lax.dynamic_slice_in_dim(kv_ext[0], block_first, block_len + 2 * WIN, 0)
        value_blk = lax.dynamic_slice_in_dim(kv_ext[1], block_first, block_len + 2 * WIN, 0)
        query_pos = device_offset + block_first + jnp.arange(block_len, dtype=jnp.int32)
        key_pos = (
            device_offset + block_first - WIN + jnp.arange(block_len + 2 * WIN, dtype=jnp.int32)
        )
        return attend_block(query_blk, key_blk, value_blk, sink_logits, query_pos, key_pos, seq_len)

    blocks = lax.map(one_block, jnp.arange(tok_local // block_len, dtype=jnp.int32))
    attended = blocks.reshape(tok_local, queries.shape[1])
    own_first = lax.axis_index("tp") * share_rows
    attn_full = lax.psum(
        jnp.dot(attended, out_weight, preferred_element_type=jnp.float32).astype(jnp.bfloat16), "tp"
    ).astype(jnp.float32)
    middle_all = residual.astype(jnp.float32) + attn_full
    normed_all = rms_scale(middle_all, norm_gain)
    middle_own = lax.dynamic_slice_in_dim(middle_all, own_first, share_rows, 0)
    gate_sectioned = lax.all_gather(gate_weight, "sp", axis=0, tiled=True)
    up_sectioned = lax.all_gather(up_weight, "sp", axis=0, tiled=True)
    gate_acc = jnp.dot(normed_all, gate_sectioned, preferred_element_type=jnp.float32)
    up_acc = jnp.dot(normed_all, up_sectioned, preferred_element_type=jnp.float32)
    down_whole = lax.all_gather(down_weight, "sp", axis=1, tiled=True)
    hidden = (jax.nn.silu(gate_acc) * up_acc).astype(jnp.bfloat16)
    ffn_share = lax.psum_scatter(
        jnp.dot(hidden, down_whole, preferred_element_type=jnp.float32).astype(jnp.bfloat16),
        "tp",
        scatter_dimension=0,
        tiled=True,
    ).astype(jnp.float32)
    return (middle_own + ffn_share).astype(jnp.bfloat16)


def shards(
    queries,
    key_rows,
    value_rows,
    sink_logits,
    residual,
    norm_gain,
    out_weight,
    gate_weight,
    up_weight,
    down_weight,
):
    n_sp, n_tp = lax.axis_size("sp"), lax.axis_size("tp")
    if n_sp % 4 or n_tp % 2 or down_weight.shape[1] % (2 * LANES):
        return gathered(
            queries,
            key_rows,
            value_rows,
            sink_logits,
            residual,
            norm_gain,
            out_weight,
            gate_weight,
            up_weight,
            down_weight,
        )
    lay = Layout(n_sp, n_tp)
    far_n, ranks = lay.far, lay.ranks
    f32, bf16 = jnp.float32, jnp.bfloat16
    s, t = lax.axis_index("sp"), lax.axis_index("tp")
    far, near, side, core = s // 4, (s // 2) % 2, s % 2, t % 2
    tok_local = queries.shape[0]
    share = tok_local // n_tp
    width = residual.shape[1]
    steps = [(a, e) for a in range(far_n) for e in range(2)]

    kv_ext = halo(jnp.stack([key_rows, value_rows]))

    half_rows = gate_weight.shape[0] // 2
    to_dest = {
        (a, e): lay.pairs(lambda f, n, d, r, c, a=a, e=e: ((f - a) % far_n, c, d, r, n ^ e))
        for a, e in steps
    }
    to_side = lay.pairs(lambda f, n, d, r, c: (f, n, d ^ 1, r, c))
    to_core = lay.pairs(lambda f, n, d, r, c: (f, n, d, r, c ^ 1))
    to_near = lay.pairs(lambda f, n, d, r, c: (f, n ^ 1, d, r, c))

    def spread(pieces):
        out = []
        for a, e in steps:
            mine = send(pieces[e], to_dest[a, e])
            other = send(mine, to_side)
            out.append([mine, other, send(mine, to_core), send(other, to_core)])
        return out

    gu_parts = []
    for e in range(2):
        first = (near ^ e) * half_rows
        gu_parts.append(
            jnp.stack(
                [lax.dynamic_slice_in_dim(w, first, half_rows, 0) for w in (gate_weight, up_weight)]
            )
        )
    gu = spread(gu_parts)

    block_len = 2 * WIN
    seq_len = tok_local * n_sp
    device_offset = s * tok_local
    blocks = []
    for index in range(tok_local // block_len):
        first = index * block_len
        query_pos = device_offset + first + jnp.arange(block_len, dtype=jnp.int32)
        key_pos = device_offset + first - WIN + jnp.arange(block_len + 2 * WIN, dtype=jnp.int32)
        blocks.append(
            attend_block(
                queries[first : first + block_len],
                kv_ext[0, first : first + block_len + 2 * WIN],
                kv_ext[1, first : first + block_len + 2 * WIN],
                sink_logits,
                query_pos,
                key_pos,
                seq_len,
            )
        )
    attended = jnp.concatenate(blocks, axis=0)
    partial = jnp.dot(attended, out_weight, preferred_element_type=f32).astype(bf16)
    partial = partial.reshape(ranks, 2, share, width)
    keep = lax.dynamic_index_in_dim(partial, core, 1, keepdims=False)
    give = lax.dynamic_index_in_dim(partial, 1 - core, 1, keepdims=False)
    chip_sum = keep.astype(f32) + send(give, to_core).astype(f32)
    rank = t // 2
    own = lax.dynamic_index_in_dim(chip_sum, rank, 0, keepdims=False)
    for k in range(1, ranks):
        to_rank = lay.pairs(lambda f, n, d, r, c, k=k: (f, n, d, (r + k) % ranks, c))
        theirs = lax.dynamic_index_in_dim(chip_sum, (rank + k) % ranks, 0, keepdims=False)
        own = own + send(theirs.astype(bf16), to_rank).astype(f32)
    middle = lax.dynamic_slice_in_dim(residual, t * share, share, 0).astype(f32) + own
    normed = rms_scale(middle, norm_gain)

    order = []
    for a, e in steps:
        for c in (core, 1 - core):
            for b in range(2):
                order.append(((((far + a) % far_n) * 2 + (c ^ e)) * 2 + (side ^ b)) * 2 + c)
    normed = jnp.concatenate(
        [lax.dynamic_slice_in_dim(normed, p * half_rows, half_rows, 1) for p in order], axis=1
    )
    down_parts = []
    half_cols = down_weight.shape[1] // 2
    down_tied, normed = lax.optimization_barrier((down_weight, normed))
    for e in range(2):
        down_parts.append(
            lax.dynamic_slice_in_dim(down_tied, (near ^ e) * half_cols, half_cols, 1)
        )
    by_rank = [normed]
    rank_moves = [
        lay.pairs(lambda f, n, d, r, c, k=k: (f, n, d, (r - k) % ranks, c)) for k in range(ranks)
    ]
    near_rows = send(normed, to_near)
    for k in range(1, ranks):
        by_rank.append(send(normed, rank_moves[k]))
    by_rank.append(near_rows)
    for k in range(1, ranks):
        by_rank.append(send(near_rows, rank_moves[k]))
    rows = jnp.concatenate(by_rank, axis=0)

    down = spread(down_parts)

    step_cols = 4 * half_rows
    gate_acc = up_acc = None
    for k, got in enumerate(gu):
        part = rows[:, k * step_cols : (k + 1) * step_cols]
        gate = jnp.dot(
            part, jnp.concatenate([g[0] for g in got], axis=0), preferred_element_type=f32
        )
        up = jnp.dot(part, jnp.concatenate([g[1] for g in got], axis=0), preferred_element_type=f32)
        gate_acc = gate if gate_acc is None else gate_acc + gate
        up_acc = up if up_acc is None else up_acc + up
    hidden = (jax.nn.silu(gate_acc) * up_acc).astype(bf16)

    sums = []
    for got in down:
        part = jnp.dot(hidden, jnp.concatenate(got, axis=1), preferred_element_type=f32)
        part = part.astype(bf16).reshape(2, ranks, share, part.shape[1])
        total = part[:, 0].astype(f32)
        for k in range(1, ranks):
            back = lay.pairs(lambda f, n, d, r, c, k=k: (f, n, d, (r + k) % ranks, c))
            total = total + send(part[:, k], back).astype(f32)
        sums.append(total[0] + send(total[1].astype(bf16), to_near).astype(f32))
    ffn = jnp.concatenate(sums, axis=1)

    back_order = []
    for j in range(2 * n_sp):
        sj, h = j // 2, j % 2
        mate = h ^ core
        a = (sj // 4 - far) % far_n
        e = ((sj // 2) % 2) ^ h
        b = (sj % 2) ^ side
        back_order.append((a * 2 + e) * 4 + mate * 2 + b)
    ffn = jnp.concatenate(
        [lax.dynamic_slice_in_dim(ffn, p * half_cols, half_cols, 1) for p in back_order], axis=1
    )
    return (middle + ffn).astype(bf16)


def solution(mesh):
    placed = (
        P("sp", "tp"),
        P("sp", "tp"),
        P("sp", "tp"),
        P("tp"),
        P("sp", None),
        P(),
        P("tp", None),
        P("sp", "tp"),
        P("sp", "tp"),
        P("tp", "sp"),
    )
    return jax.shard_map(
        shards, mesh=mesh, in_specs=placed, out_specs=P(("sp", "tp"), None), check_vma=False
    )
```
